32 devices in a mesh: grp: 2 (over x), ep: 16 (over z, y, core).
Axes of the slice: x: 2, y: 2, z: 4, core: 2. Of those that a mesh axis runs over, the one named last changes fastest.
Arguments:
- tokens: bfloat16 [32, 2048], P(('grp', 'ep')), parts along dimension 0, may hold values from -6 to 6
- cache_latent: bfloat16 [32, 3072, 512], P(('grp', 'ep')), parts along dimension 0, may hold values from -6 to 6
- cache_rope: bfloat16 [32, 32, 3072], P(('grp', 'ep')), parts along dimension 0, may hold values from -1000 to 1000
- lengths: int32 [32], P(('grp', 'ep')), parts along dimension 0, may hold values from 384 to 3072, as said below
- w_query: bfloat16 [2048, 1536], P('ep'), may hold values from -0.125 to 0.125
- w_latent: bfloat16 [2048, 512], P('ep'), may hold values from -0.125 to 0.125
- w_rope: bfloat16 [2048, 32], P('ep'), may hold values from -0.125 to 0.125
- w_absorb: bfloat16 [512, 1024], replicated, may hold values from -0.25 to 0.25
- w_value: bfloat16 [512, 1024], replicated, may hold values from -0.25 to 0.25
- w_output: bfloat16 [1024, 2048], P('ep'), may hold values from -0.1875 to 0.1875
- gain_attn: float32 [2048], replicated, may hold values from 0.1 to 1.9
- gain_latent: float32 [512], replicated, may hold values from 0.1 to 1.9
- gain_moe: float32 [2048], replicated, may hold values from 0.1 to 1.9
- routes: int32 [32, 2], P(('grp', 'ep')), parts along dimension 0, may hold values from 0 to 15, all different within a row; in each aligned block of 16 rows (0 to 15, 16 to 31, ...) at most 4 rows name the same one
- route_scores: float32 [32, 2], P(('grp', 'ep')), parts along dimension 0, may hold values from 0.2 to 1
- w_gate: bfloat16 [16, 2048, 512], P('ep'), may hold values from -0.125 to 0.125
- w_up: bfloat16 [16, 2048, 512], P('ep'), may hold values from -0.125 to 0.125
- w_down: bfloat16 [16, 512, 2048], P('ep'), may hold values from -0.25 to 0.25
Outputs:
- mixed: bfloat16 [32, 2048], P(('grp', 'ep')), parts along dimension 0
- new_latent: bfloat16 [32, 512], P(('grp', 'ep')), parts along dimension 0
- new_rope: bfloat16 [32, 32], P(('grp', 'ep')), parts along dimension 0
The draws below stay inside these ranges and needn't reach their ends.
There are 2 independent parts, one for each index of `grp`. The reference program is written for one: setup_inputs(seed, part) draws one part's arguments, and reference() takes and returns one part's arrays. A program takes and returns all parts, laid end to end along the dimension named above; an argument that names none is the same for every part. Nothing has to cross between parts.
Inputs may be any that keep to these rules, and one draw needn't show every extreme that they name: `routes`: each row names 2 different experts; over one part's 16 tokens no expert is named by more than 4 rows, a bound that some block reaches. `lengths`: some sequence has all 3072 positions filled.
All inputs are finite; a program needn't handle non-finite values.
Results may differ from the reference program's by a relative error of at most 0.013.
Values may be sent and summed in bfloat16 or wider, within the bound.
A program may use at most 64 MiB of HBM per device.

```python
import math
import jax
import jax.numpy as jnp
import numpy as np
from jax import lax

D = 2048
HEADS = 16
NOPE = 64
ROPE = 32
VDIM = 64
LATENT = 512
FF = 512
TOPK = 2
CACHE = 3072
SEQS = 16
EXPERTS = 16
CAP = 4


def draw_cache_rope(key, part):
    k_base = jax.random.fold_in(jax.random.fold_in(key, 31), 0)
    base = jnp.clip(jax.random.normal(k_base, (SEQS, ROPE, CACHE), jnp.float32), -6.0, 6.0)
    return base.astype(jnp.bfloat16)


def draw_lengths(key, part):
    k_len, k_full = jax.random.split(jax.random.fold_in(key, 23))
    values = jax.random.randint(k_len, (SEQS,), CACHE // 8, CACHE + 1)
    chosen = jax.random.randint(k_full, (), 0, SEQS)
    values = jnp.where(jnp.arange(SEQS) == chosen, CACHE, values)
    return values.astype(jnp.int32)


def block_scale(own_key, extent, shards, low, top_value):
    def one(dim, shards_of):
        draws = jax.random.uniform(jax.random.fold_in(jax.random.fold_in(own_key, 6), dim), (shards_of,), jnp.float32, low / len(shards), top_value / len(shards))
        return jnp.repeat(jnp.exp(draws), extent[dim] // shards_of).reshape((-1,) + (1,) * (len(extent) - dim - 1))

    level = one(*shards[0])
    for cut in shards[1:]:
        level = level * one(*cut)
    return level


def assign_block(own_key, own, number, rows, number_of, top, most, lean):
    order = jax.random.permutation(own_key, number_of)
    crowded, ordinary = portions_of(number_of, rows * top, most, lean, True), portions_of(number_of, rows * top, most, lean, False)
    places = jnp.arange(number_of)

    def named(sizes, turn):
        used = int((sizes > 0).sum())
        fixed = max(1, used // 4)
        moved = fixed + (places - fixed + turn * (used - fixed)) % max(1, number_of - fixed)
        return jnp.zeros((number_of,), jnp.int32).at[order[jnp.where(places < fixed, places, moved)]].set(jnp.asarray(sizes, jnp.int32))

    sizes = jnp.where(number % 4 == 0, named(crowded, number // 4), named(ordinary, number - number // 4 - 1))
    mixed = jax.random.permutation(jax.random.fold_in(own, 3), number_of)
    donor, receiver = mixed[0:number_of // 2 * 2:2], mixed[1:number_of // 2 * 2:2]
    margin = jnp.minimum(sizes[donor] - 1, most - sizes[receiver]) // 2
    margin = jnp.where((donor == order[0]) | (receiver == order[0]) | (sizes[receiver] == 0), 0, jnp.maximum(margin, 0))
    moved = jax.random.randint(jax.random.fold_in(own, 4), (number_of // 2,), 0, 1 << 20) % (margin + 1)
    sizes = sizes.at[donor].add(-moved).at[receiver].add(moved)
    items = jnp.searchsorted(jnp.cumsum(sizes), jnp.arange(rows * top), side="right").astype(jnp.int32)
    table = items.reshape(top, rows).T
    table = table[jax.random.permutation(jax.random.fold_in(own, 1), rows)]
    turn = jax.random.randint(jax.random.fold_in(own, 2), (rows, 1), 0, top)
    return jnp.take_along_axis(table, (jnp.arange(top)[None, :] + turn) % top, axis=1)


def portions_of(number_of, total, bound, lean, full):
    portions = [(1 << 20) // math.isqrt(grade ** lean) + 1 for grade in range(1, number_of + 1)]
    largest = bound if full else min(bound, max(-(-total // number_of), total * portions[0] // sum(portions)))
    least = 1 if total - largest >= number_of - 1 else 0
    given, spare = [largest] + [least] * (number_of - 1), total - largest - least * (number_of - 1)
    while spare > 0:
        free = [i for i in range(1, number_of) if given[i] < largest] or [i for i in range(1, number_of) if given[i] < bound]
        whole, remaining = sum([portions[i] for i in free]), spare
        for i in free:
            extra = min(bound - given[i], max(1, remaining * portions[i] // whole), spare)
            given[i] = given[i] + extra
            spare = spare - extra
    return np.array(given)


def scatter_about(stream_key, shape, scale, reach, cuts=(), held_as=jnp.bfloat16):
    array = jax.random.normal(stream_key, shape, jnp.float32) * scale
    if len(cuts) > 0:
        array = block_scale(stream_key, shape, cuts, -0.22, 0.18) * array
    return jnp.clip(array, min=-reach, max=reach).astype(held_as)


def setup_inputs(seed: int = 0, part: int = 0) -> dict:
    streams_of = jax.random.split(jax.random.key(seed), 19)
    own_keys = jax.random.split(jax.random.fold_in(streams_of[18], part), 19)
    tokens = scatter_about(own_keys[0], (SEQS, D), 1.0, 6.0, ((0, 16),))
    cache_latent = scatter_about(own_keys[1], (SEQS, CACHE, LATENT), 1.0, 6.0, ((0, 16),))
    cache_rope = draw_cache_rope(jax.random.fold_in(jax.random.fold_in(streams_of[18], part), 71), part)
    lengths = draw_lengths(jax.random.fold_in(jax.random.fold_in(streams_of[18], part), 71), part)
    w_query = scatter_about(streams_of[4], (D, HEADS * (NOPE + ROPE)), D ** -0.5, 0.125, ((0, 16),))
    w_latent = scatter_about(streams_of[5], (D, LATENT), D ** -0.5, 0.125, ((0, 16),))
    w_rope = scatter_about(streams_of[6], (D, ROPE), D ** -0.5, 0.125, ((0, 16),))
    w_absorb = scatter_about(streams_of[7], (LATENT, HEADS * NOPE), LATENT ** -0.5, 0.25)
    w_value = scatter_about(streams_of[8], (LATENT, HEADS * VDIM), LATENT ** -0.5, 0.25)
    w_output = scatter_about(streams_of[9], (HEADS * VDIM, D), (HEADS * VDIM) ** -0.5, 0.1875, ((0, 16),))
    gain_attn = jnp.clip(1.0 + 0.18 * jax.random.normal(streams_of[10], (D,), jnp.float32), 0.1, 1.9)
    gain_latent = jnp.clip(1.0 + 0.18 * jax.random.normal(streams_of[11], (LATENT,), jnp.float32), 0.1, 1.9)
    gain_moe = jnp.clip(1.0 + 0.18 * jax.random.normal(streams_of[12], (D,), jnp.float32), 0.1, 1.9)
    routes_keys = jax.random.split(jax.random.fold_in(own_keys[13], 1), SEQS // SEQS)
    routes_turns = jax.random.permutation(jax.random.fold_in(own_keys[13], 3), SEQS // SEQS)
    routes = jax.vmap(lambda own, number: assign_block(jax.random.fold_in(own_keys[13], 2), own, number, SEQS, EXPERTS, TOPK, CAP, 2))(routes_keys, routes_turns).reshape((SEQS, TOPK))
    route_scores = jnp.clip(jnp.exp(math.log(1.0) - 1.609438 * jax.random.uniform(own_keys[14], (SEQS, TOPK), jnp.float32) ** block_scale(own_keys[14], (SEQS, TOPK), ((0, 16),), -0.2, 0.2)), 0.2, 1.0)
    w_gate = scatter_about(streams_of[15], (EXPERTS, D, FF), D ** -0.5, 0.125, ((0, 16),))
    w_up = scatter_about(streams_of[16], (EXPERTS, D, FF), D ** -0.5, 0.125, ((0, 16),))
    w_down = scatter_about(streams_of[17], (EXPERTS, FF, D), FF ** -0.5, 0.25, ((0, 16),))
    return {"tokens": tokens, "cache_latent": cache_latent, "cache_rope": cache_rope, "lengths": lengths, "w_query": w_query, "w_latent": w_latent, "w_rope": w_rope, "w_absorb": w_absorb, "w_value": w_value, "w_output": w_output, "gain_attn": gain_attn, "gain_latent": gain_latent, "gain_moe": gain_moe, "routes": routes, "route_scores": route_scores, "w_gate": w_gate, "w_up": w_up, "w_down": w_down}


EPS = 1e-06
THETA = 10000.0

def rms_scale(values, gain):
    return values * lax.rsqrt(lax.optimization_barrier(jnp.mean(values * values, axis=-1, keepdims=True)) + EPS) * gain.astype(jnp.float32)

def rope_tables(positions, width):
    inverse = THETA ** (-jnp.arange(0, width, 2).astype(jnp.float32) / width)
    angle = positions.astype(jnp.float32)[:, None] * inverse[None, :]
    return (jnp.cos(angle), jnp.sin(angle))

def apply_rope(values, cosine, sine):
    half = values.shape[-1] // 2
    first, second = (values[..., :half], values[..., half:])
    return jnp.concatenate([first * cosine - second * sine, second * cosine + first * sine], axis=-1)

def attend_one(items):
    q_abs, q_pe, lat_cache, rope_cache, ckv, kpe, length = items
    scale = (NOPE + ROPE) ** (-0.5)
    past = (jnp.einsum('hc,kc->hk', q_abs.astype(jnp.float32), lat_cache.astype(jnp.float32)) + jnp.einsum('hr,rk->hk', q_pe.astype(jnp.float32), rope_cache.astype(jnp.float32))) * scale
    fresh = (jnp.einsum('hc,c->h', q_abs.astype(jnp.float32), ckv.astype(jnp.float32)) + jnp.einsum('hr,r->h', q_pe.astype(jnp.float32), kpe.astype(jnp.float32))) * scale
    valid = jnp.arange(lat_cache.shape[0]).astype(jnp.int32)[None, :] < length
    top = jnp.maximum(lax.optimization_barrier(jnp.max(jnp.where(valid, past, -jnp.inf), axis=-1)), fresh)
    e_past = jnp.where(valid, jnp.exp(past - top[:, None]), 0.0)
    e_new = jnp.exp(fresh - top)
    total = lax.optimization_barrier(jnp.sum(e_past, axis=-1)) + e_new
    p_past = (e_past / total[:, None]).astype(jnp.bfloat16)
    p_new = (e_new / total).astype(jnp.bfloat16)
    out = jnp.einsum('hk,kc->hc', p_past.astype(jnp.float32), lat_cache.astype(jnp.float32)) + p_new.astype(jnp.float32)[:, None] * ckv.astype(jnp.float32)[None, :]
    return out.astype(jnp.bfloat16)

def reference(tokens, cache_latent, cache_rope, lengths, w_query, w_latent, w_rope, w_absorb, w_value, w_output, gain_attn, gain_latent, gain_moe, routes, route_scores, w_gate, w_up, w_down):
    count = tokens.shape[0]
    normed = rms_scale(tokens.astype(jnp.float32), gain_attn).astype(jnp.bfloat16)
    query = jnp.dot(normed, w_query, preferred_element_type=jnp.float32).astype(jnp.bfloat16)
    latent_raw = jnp.dot(normed, w_latent, preferred_element_type=jnp.float32).astype(jnp.bfloat16)
    rope_raw = jnp.dot(normed, w_rope, preferred_element_type=jnp.float32).astype(jnp.bfloat16)
    new_latent = rms_scale(latent_raw.astype(jnp.float32), gain_latent).astype(jnp.bfloat16)
    cosine, sine = rope_tables(lengths, ROPE)
    new_rope = apply_rope(rope_raw.astype(jnp.float32), cosine, sine).astype(jnp.bfloat16)
    heads_view = query.reshape(count, HEADS, NOPE + ROPE)
    q_nope = heads_view[:, :, :NOPE]
    q_pe = apply_rope(heads_view[:, :, NOPE:].astype(jnp.float32), cosine[:, None, :], sine[:, None, :]).astype(jnp.bfloat16)
    q_abs = jnp.einsum('shn,chn->shc', q_nope.astype(jnp.float32), w_absorb.reshape(LATENT, HEADS, NOPE).astype(jnp.float32)).astype(jnp.bfloat16)
    attended = lax.map(attend_one, (q_abs, q_pe, cache_latent, cache_rope, new_latent, new_rope, lengths))
    values = jnp.einsum('shc,chv->shv', attended.astype(jnp.float32), w_value.reshape(LATENT, HEADS, VDIM).astype(jnp.float32)).astype(jnp.bfloat16)
    attn_out = jnp.dot(values.reshape(count, HEADS * VDIM), w_output, preferred_element_type=jnp.float32)
    resid = (tokens.astype(jnp.float32) + attn_out).astype(jnp.bfloat16)
    moe_in = rms_scale(resid.astype(jnp.float32), gain_moe).astype(jnp.bfloat16)

    def expert_one(items):
        index, row = items
        gate = jnp.dot(row[None, :], w_gate[index], preferred_element_type=jnp.float32)
        upper = jnp.dot(row[None, :], w_up[index], preferred_element_type=jnp.float32)
        hidden = (jax.nn.silu(gate) * upper).astype(jnp.bfloat16)
        return jnp.dot(hidden, w_down[index], preferred_element_type=jnp.float32).astype(jnp.bfloat16)[0]
    flat_ids = routes.reshape(-1).astype(jnp.int32)
    flat_rows = jnp.repeat(moe_in, TOPK, axis=0)
    expert_out = lax.map(expert_one, (flat_ids, flat_rows)).reshape(count, TOPK, D)
    route_weight = route_scores / lax.optimization_barrier(jnp.sum(route_scores, axis=-1, keepdims=True))
    moe_sum = lax.optimization_barrier(jnp.sum(route_weight[:, :, None] * expert_out.astype(jnp.float32), axis=1))
    mixed = (resid.astype(jnp.float32) + moe_sum).astype(jnp.bfloat16)
    return (mixed, new_latent, new_rope)
```

```python
import functools
import jax
import jax.numpy as jnp
from jax import lax
from jax.experimental import pallas as pl
from jax.experimental.pallas import tpu as pltpu
from jax.sharding import PartitionSpec as P

HEADS = 16
NOPE = 64
ROPE = 32
VDIM = 64
EPS = 1e-06
THETA = 10000.0
LANES = 128
F32 = jnp.float32
BF16 = jnp.bfloat16
MESH = pl.DeviceIdType.MESH


def dot(a, b):
    return jnp.dot(a, b, preferred_element_type=F32)


def dot_t(a, b):
    return lax.dot_general(a, b, (((1,), (1,)), ((), ())), preferred_element_type=F32)


def rms_scale(values, gain):
    return values * lax.rsqrt(jnp.mean(values * values, axis=-1, keepdims=True) + EPS) * gain


def iota(shape, dim):
    return lax.broadcasted_iota(jnp.int32, shape, dim)


def ones_where(mask):
    return jnp.where(mask, 1.0, 0.0).astype(BF16)


def kernel(
    n,
    tok_ref, table_ref, g_attn_ref, g_lat_ref, g_moe_ref, len_ref, route_ref, score_ref,
    cache_hbm, crope_hbm, wq_hbm, wl_hbm, wr_hbm, wa_hbm, wv_hbm, wo_hbm, wg_hbm, wu_hbm, wd_hbm,
    mixed_ref, nlat_ref, nrope_ref,
    cache, crope, wq, wl, wr, wa, wv, wo, wg, wu, wd,
    send1, recv1, rows1, send2, recv2, send3, recv3, rows3, send4, recv4, send5, recv5, rows5,
    send6, recv6, local_sem, link_sem,
):
    me = lax.axis_index("ep")
    pairs = [
        (wq_hbm, wq), (wl_hbm, wl), (wr_hbm, wr), (wa_hbm, wa), (crope_hbm.at[0], crope),
        (cache_hbm.at[0], cache), (wv_hbm, wv), (wo_hbm, wo),
        (wg_hbm.at[0], wg), (wu_hbm.at[0], wu), (wd_hbm.at[0], wd),
    ]
    loads = [pltpu.make_async_copy(a, b, local_sem.at[i]) for i, (a, b) in enumerate(pairs)]
    for load in loads:
        load.start()
    (l_wq, l_wl, l_wr, l_wa, l_crope, l_cache, l_wv, l_wo, l_wg, l_wu, l_wd) = loads

    barrier = pltpu.get_barrier_semaphore()

    def greet(k, carry):
        pl.semaphore_signal(
            barrier, inc=1, device_id={"ep": lax.rem(me + k, n)}, device_id_type=MESH
        )
        return carry

    lax.fori_loop(1, n, greet, 0)

    def copy(phase, source, target, peer, slot):
        return pltpu.make_async_remote_copy(
            src_ref=source(peer),
            dst_ref=target.at[slot],
            send_sem=link_sem.at[phase, 0, peer],
            recv_sem=link_sem.at[phase, 1, slot],
            device_id={"ep": peer},
            device_id_type=MESH,
        )

    def send(phase, source, target):
        def step(k, carry):
            copy(phase, source, target, lax.rem(me + k, n), me).start()
            return carry

        lax.fori_loop(1, n, step, 0)

    def receive(phase, source, target):
        def step(k, carry):
            peer = lax.rem(me + n - k, n)
            copy(phase, source, target, peer, peer).wait_recv()
            return carry

        lax.fori_loop(1, n, step, 0)

    def sent(phase, source, target):
        def step(k, carry):
            peer = lax.rem(me + k, n)
            copy(phase, source, target, peer, peer).wait_send()
            return carry

        lax.fori_loop(1, n, step, 0)

    def gather_rows(buffer, rows):
        for t in range(n):
            rows[t : t + 1, :] = buffer[t]

    tokens = tok_ref[...].astype(F32)
    normed = rms_scale(tokens, g_attn_ref[...]).astype(BF16).astype(F32)
    depth = wq.shape[0]
    for t in range(n):
        send1[t] = normed[:, t * depth : (t + 1) * depth]
    recv1[me] = send1[me]
    pl.semaphore_wait(barrier, n - 1)
    src1 = lambda peer: send1.at[peer]
    send(0, src1, recv1)
    qw, lw, rw = wq.shape[1], wl.shape[1], wr.shape[1]
    l_wq.wait()
    l_wl.wait()
    l_wr.wait()
    receive(0, src1, recv1)
    gather_rows(recv1, rows1)
    rows = rows1[...].astype(BF16)
    part_q = dot(rows, wq[...])
    part_l = dot(rows, wl[...])
    part_r = dot(rows, wr[...])
    for t in range(n):
        send2[t, :, :qw] = part_q[t : t + 1]
        send2[t, :, qw : qw + lw] = part_l[t : t + 1]
        send2[t, :, qw + lw : qw + lw + rw] = part_r[t : t + 1]
    recv2[me] = send2[me]
    src2 = lambda peer: send2.at[peer]
    send(1, src2, recv2)
    sel = jnp.concatenate([ones_where(iota((NOPE + ROPE, LANES), 0) == iota((NOPE + ROPE, LANES), 1))] * HEADS, axis=0)
    head_width = NOPE + ROPE
    own_q = iota((HEADS, qw), 1) - head_width * iota((HEADS, qw), 0)
    own_q = (own_q >= 0) & (own_q < head_width)
    spread = ones_where((iota((LANES, HEADS * NOPE), 1) & (NOPE - 1)) == iota((LANES, HEADS * NOPE), 0))
    own_n = iota((HEADS, HEADS * NOPE), 1) - NOPE * iota((HEADS, HEADS * NOPE), 0)
    own_n = (own_n >= 0) & (own_n < NOPE)
    half = ROPE // 2
    lane = iota((LANES, ROPE), 1)
    swapped = jnp.where(lane < half, lane + half, lane - half)
    pick = ones_where(iota((LANES, ROPE), 0) == NOPE + lane)
    pick_swap = ones_where(iota((LANES, ROPE), 0) == NOPE + swapped)
    swap = ones_where(iota((ROPE, ROPE), 0) == swapped[:ROPE])
    cosine, sine = table_ref[0:1, :], table_ref[1:2, :]
    receive(1, src2, recv2)
    summed = jnp.sum(recv2[:, :, : qw + lw + LANES], axis=0)
    latent_raw = summed[:, qw : qw + lw].astype(BF16).astype(F32)
    new_latent = rms_scale(latent_raw, g_lat_ref[...]).astype(BF16)
    nlat_ref[...] = new_latent
    new_latent = new_latent.astype(F32)
    rope_raw = jnp.broadcast_to(summed[:, qw + lw : qw + lw + rw].astype(BF16).astype(F32), (HEADS, rw))
    new_rope = rope_raw * cosine + dot(rope_raw.astype(BF16), swap) * sine
    new_rope = new_rope.astype(BF16)
    nrope_ref[...] = new_rope[0:1, :]
    new_rope = new_rope.astype(F32)
    query = jnp.broadcast_to(summed[:, :qw].astype(BF16).astype(F32), (HEADS, qw))
    query = jnp.where(own_q, query, 0.0).astype(BF16)
    heads = dot(query, sel).astype(BF16)
    q_pe = (dot(heads, pick) * cosine + dot(heads, pick_swap) * sine).astype(BF16)
    q_diag = jnp.where(own_n, dot(heads, spread), 0.0).astype(BF16)
    l_wa.wait()
    q_abs = dot_t(q_diag, wa[...]).astype(BF16)
    scale = (NOPE + ROPE) ** (-0.5)
    l_crope.wait()
    l_cache.wait()
    past = (dot_t(q_abs, cache[...]) + dot(q_pe, crope[...])) * scale
    fresh = (
        jnp.sum(q_abs.astype(F32) * new_latent, axis=-1, keepdims=True)
        + jnp.sum(q_pe.astype(F32) * new_rope, axis=-1, keepdims=True)
    ) * scale
    past = jnp.where(iota(past.shape, 1) < len_ref[0], past, -jnp.inf)
    top = jnp.maximum(jnp.max(past, axis=-1, keepdims=True), fresh)
    e_past = jnp.exp(past - top)
    e_new = jnp.exp(fresh - top)
    total = jnp.sum(e_past, axis=-1, keepdims=True) + e_new
    inverse = 1.0 / total
    p_past = (e_past * inverse).astype(BF16)
    p_new = (e_new * inverse).astype(BF16).astype(F32)
    attended = (dot(p_past, cache[...]) + p_new * new_latent).astype(BF16)
    l_wv.wait()
    values = dot(attended, wv[...])
    values = jnp.sum(jnp.where(own_n, values, 0.0), axis=0, keepdims=True).astype(BF16).astype(F32)
    for t in range(send3.shape[0]):
        send3[t] = values[:, t * LANES : (t + 1) * LANES]
    width = wo.shape[0]
    group = LANES // width
    recv3[me] = send3[me // group]
    src3 = lambda peer: send3.at[peer // group]
    send(2, src3, recv3)
    l_wo.wait()
    cut = ones_where(iota((LANES, width), 0) == iota((LANES, width), 1) + width * lax.rem(me, group))
    receive(2, src3, recv3)
    gather_rows(recv3, rows3)
    rows = dot(rows3[...].astype(BF16), cut).astype(BF16)
    part = dot(rows, wo[...])
    for t in range(n):
        send4[t] = part[t : t + 1]
    recv4[me] = send4[me]
    src4 = lambda peer: send4.at[peer]
    send(3, src4, recv4)
    receive(3, src4, recv4)
    resid = (tokens + jnp.sum(recv4[...], axis=0)).astype(BF16).astype(F32)
    moe_in = rms_scale(resid, g_moe_ref[...]).astype(BF16).astype(F32)
    send5[0] = moe_in
    recv5[me] = moe_in
    src5 = lambda peer: send5.at[0]
    send(4, src5, recv5)
    l_wg.wait()
    l_wu.wait()
    l_wd.wait()
    receive(4, src5, recv5)
    gather_rows(recv5, rows5)
    rows = rows5[...].astype(BF16)
    gate = dot(rows, wg[...])
    upper = dot(rows, wu[...])
    hidden = (jax.nn.silu(gate) * upper).astype(BF16)
    result = dot(hidden, wd[...]).astype(BF16).astype(F32)
    for t in range(n):
        send6[t] = result[t : t + 1]
    recv6[me] = send6[me]
    src6 = lambda peer: send6.at[peer]
    send(5, src6, recv6)
    topk = route_ref.shape[1]
    weight = score_ref[0, 0]
    for k in range(1, topk):
        weight = weight + score_ref[0, k]
    receive(5, src6, recv6)
    moe_sum = jnp.zeros_like(resid)
    for k in range(topk):
        moe_sum = moe_sum + (jnp.full(resid.shape, score_ref[0, k]) / weight) * recv6[route_ref[0, k]]
    mixed_ref[...] = (resid + moe_sum).astype(BF16)
    sent(0, src1, recv1)
    sent(1, src2, recv2)
    sent(2, src3, recv3)
    sent(3, src4, recv4)
    sent(4, src5, recv5)
    sent(5, src6, recv6)


def body(
    tokens, cache_latent, cache_rope, lengths, w_query, w_latent, w_rope, w_absorb, w_value,
    w_output, gain_attn, gain_latent, gain_moe, routes, route_scores, w_gate, w_up, w_down,
):
    n = lax.axis_size("ep")
    d = tokens.shape[1]
    total = w_query.shape[1] + w_latent.shape[1] + LANES
    inverse = THETA ** (-jnp.arange(0, ROPE, 2).astype(F32) / ROPE)
    angle = lengths.astype(F32)[:, None] * inverse[None, :]
    cosine, sine = jnp.cos(angle), jnp.sin(angle)
    table = jnp.concatenate(
        [jnp.concatenate([cosine, cosine], axis=1), jnp.concatenate([-sine, sine], axis=1)], axis=0
    )
    vmem = pl.BlockSpec(memory_space=pltpu.VMEM)
    smem = pl.BlockSpec(memory_space=pltpu.SMEM)
    hbm = pl.BlockSpec(memory_space=pl.ANY)

    def like(a):
        return pltpu.VMEM(a.shape[-2:], a.dtype)

    big = [w_query, w_latent, w_rope, w_absorb, w_value, w_output, w_gate, w_up, w_down]
    depth = w_query.shape[0]
    tiles = w_value.shape[1] // LANES
    row = lambda count, wide: pltpu.VMEM((count, 1, wide), F32)
    return pl.pallas_call(
        functools.partial(kernel, n),
        out_shape=(
            jax.ShapeDtypeStruct(tokens.shape, BF16),
            jax.ShapeDtypeStruct((1, w_latent.shape[1]), BF16),
            jax.ShapeDtypeStruct((1, w_rope.shape[1]), BF16),
        ),
        in_specs=[vmem] * 5 + [smem] * 3 + [hbm] * 11,
        out_specs=(vmem, vmem, vmem),
        scratch_shapes=[like(cache_latent), like(cache_rope)]
        + [like(a) for a in big]
        + [
            row(n, depth), row(n, depth), pltpu.VMEM((n, depth), F32),
            row(n, total), row(n, total),
            row(tiles, LANES), row(n, LANES), pltpu.VMEM((n, LANES), F32),
            row(n, d), row(n, d),
            row(1, d), row(n, d), pltpu.VMEM((n, d), F32),
            row(n, d), row(n, d),
            pltpu.SemaphoreType.DMA((11,)),
            pltpu.SemaphoreType.DMA((6, 2, n)),
        ],
        compiler_params=pltpu.CompilerParams(
            collective_id=0, has_side_effects=True, vmem_limit_bytes=56 * 1024 * 1024
        ),
    )(
        tokens, table, gain_attn[None, :], gain_latent[None, :], gain_moe[None, :], lengths, routes,
        route_scores, cache_latent, cache_rope, w_query, w_latent, w_rope, w_absorb, w_value,
        w_output, w_gate, w_up, w_down,
    )


def solution(mesh):
    rows = P(("grp", "ep"), None)
    cube = P(("grp", "ep"), None, None)
    split = P("ep", None)
    placed = (
        rows, cube, cube, P(("grp", "ep")), split, split, split, P(), P(), split, P(), P(), P(),
        rows, rows, P("ep", None, None), P("ep", None, None), P("ep", None, None),
    )
    return jax.shard_map(
        body, mesh=mesh, in_specs=placed, out_specs=(rows, rows, rows), check_vma=False
    )
```
